32 devices in a mesh: ra: 8 (over z, y), cb: 4 (over x, core).
Axes of the slice: x: 2, y: 2, z: 4, core: 2. Of those that a mesh axis runs over, the one named last changes fastest.
Arguments:
- tokens: bfloat16 [256, 3072], P(None, 'ra'), may hold values from -8 to 8, as said below
- first_gain: float32 [3072], P('ra'), may hold values from 0.1 to 1.9
- first_gate: float32 [3072, 8192], P('ra', 'cb'), may hold values from -0.109375 to 0.109375
- first_up: float32 [3072, 8192], P('ra', 'cb'), may hold values from -0.109375 to 0.109375
- first_down: float32 [8192, 3072], P('cb', 'ra'), may hold values from -0.0625 to 0.0625
- first_gate_scale: float32 [8192], P('cb'), may hold values from 0.5 to 2
- first_up_scale: float32 [8192], P('cb'), may hold values from 0.5 to 2
- first_down_scale: float32 [3072], P('ra'), may hold values from 0.5 to 2
- second_gain: float32 [3072], P('ra'), may hold values from 0.1 to 1.9
- second_gate: float32 [3072, 8192], P('ra', 'cb'), may hold values from -0.109375 to 0.109375
- second_up: float32 [3072, 8192], P('ra', 'cb'), may hold values from -0.109375 to 0.109375
- second_down: float32 [8192, 3072], P('cb', 'ra'), may hold values from -0.0625 to 0.0625
- second_gate_scale: float32 [8192], P('cb'), may hold values from 0.5 to 2
- second_up_scale: float32 [8192], P('cb'), may hold values from 0.5 to 2
- second_down_scale: float32 [3072], P('ra'), may hold values from 0.5 to 2
Outputs:
- mixed: bfloat16 [256, 3072], P(None, 'ra')
The draws below stay inside these ranges and needn't reach their ends.
Inputs may be any that keep to these rules, and one draw needn't show every extreme that they name: The features come in groups of 64 with different magnitudes, and tokens differ in magnitude.
All inputs are finite; a program needn't handle non-finite values.
Results may differ from the reference program's by a relative error of at most 0.0093.
Values may be sent and summed in bfloat16 or wider, within the bound.
A program may use at most 64 MiB of HBM per device.

```python
import math
import jax
import jax.numpy as jnp
from jax import lax

D = 3072
FF = 8192
TOKENS = 256


def draw_tokens(key, part):
    base_key = jax.random.fold_in(key, 11)
    key_list = jax.random.split(base_key, 4)
    group_scale = jnp.exp(jax.random.uniform(key_list[0], (D // 64,), jnp.float32, math.log(0.1), 0.0))
    column_scale = jnp.repeat(group_scale, 64)
    row_scale = jnp.exp(jax.random.uniform(key_list[1], (TOKENS, 1), jnp.float32, math.log(0.5), math.log(2.0)))
    base_values = jnp.clip(jax.random.normal(key_list[3], (TOKENS, D), jnp.float32), -4.0, 4.0)
    return (base_values * column_scale[None, :] * row_scale).astype(jnp.bfloat16)


def block_levels(own_key, shape, cuts, smallest, largest):
    level = 1.0
    for position, parts in cuts:
        heights = jax.random.uniform(jax.random.fold_in(jax.random.fold_in(own_key, 6), position), (parts,), jnp.float32, smallest / len(cuts), largest / len(cuts))
        level = level * jnp.repeat(jnp.exp(heights), shape[position] // parts).reshape((-1,) + (1,) * (len(shape) - 1 - position))
    return level


def scatter_about(stream_key, shape, deviation, most, cuts=(), dtype=jnp.bfloat16):
    loudness = block_levels(stream_key, shape, cuts, -0.22, 0.18) if cuts else 1.0
    array = jax.random.normal(stream_key, shape, jnp.float32) * deviation * loudness
    return jnp.minimum(jnp.maximum(array, -most), most).astype(dtype)


def setup_inputs(seed: int = 0) -> dict:
    arg_keys = jax.random.split(jax.random.key(seed), 16)
    return {
        "tokens": draw_tokens(jax.random.fold_in(arg_keys[15], 71), 0),
        "first_gain": jnp.clip(1.0 + 0.18 * jax.random.normal(arg_keys[1], (D,), jnp.float32), 0.1, 1.9),
        "first_gate": scatter_about(arg_keys[2], (D, FF), D ** -0.5, 0.109375, ((0, 8), (1, 4)), jnp.float32),
        "first_up": scatter_about(arg_keys[3], (D, FF), D ** -0.5, 0.109375, ((0, 8), (1, 4)), jnp.float32),
        "first_down": scatter_about(arg_keys[4], (FF, D), FF ** -0.5, 0.0625, ((0, 4), (1, 8)), jnp.float32),
        "first_gate_scale": jnp.clip(jnp.exp(math.log(2.0) - 1.3862944 * jax.random.uniform(arg_keys[5], (FF,), jnp.float32) ** block_levels(arg_keys[5], (FF,), ((0, 4),), -0.2, 0.2)), 0.5, 2.0),
        "first_up_scale": jnp.clip(jnp.exp(math.log(2.0) - 1.3862944 * jax.random.uniform(arg_keys[6], (FF,), jnp.float32) ** block_levels(arg_keys[6], (FF,), ((0, 4),), -0.2, 0.2)), 0.5, 2.0),
        "first_down_scale": jnp.clip(jnp.exp(math.log(2.0) - 1.3862944 * jax.random.uniform(arg_keys[7], (D,), jnp.float32) ** block_levels(arg_keys[7], (D,), ((0, 8),), -0.2, 0.2)), 0.5, 2.0),
        "second_gain": jnp.clip(1.0 + 0.18 * jax.random.normal(arg_keys[8], (D,), jnp.float32), 0.1, 1.9),
        "second_gate": scatter_about(arg_keys[9], (D, FF), D ** -0.5, 0.109375, ((0, 8), (1, 4)), jnp.float32),
        "second_up": scatter_about(arg_keys[10], (D, FF), D ** -0.5, 0.109375, ((0, 8), (1, 4)), jnp.float32),
        "second_down": scatter_about(arg_keys[11], (FF, D), FF ** -0.5, 0.0625, ((0, 4), (1, 8)), jnp.float32),
        "second_gate_scale": jnp.clip(jnp.exp(math.log(2.0) - 1.3862944 * jax.random.uniform(arg_keys[12], (FF,), jnp.float32) ** block_levels(arg_keys[12], (FF,), ((0, 4),), -0.2, 0.2)), 0.5, 2.0),
        "second_up_scale": jnp.clip(jnp.exp(math.log(2.0) - 1.3862944 * jax.random.uniform(arg_keys[13], (FF,), jnp.float32) ** block_levels(arg_keys[13], (FF,), ((0, 4),), -0.2, 0.2)), 0.5, 2.0),
        "second_down_scale": jnp.clip(jnp.exp(math.log(2.0) - 1.3862944 * jax.random.uniform(arg_keys[14], (D,), jnp.float32) ** block_levels(arg_keys[14], (D,), ((0, 8),), -0.2, 0.2)), 0.5, 2.0),
    }


def half_step(stream_in, gain, w_gate, w_up, w_down, gate_scale, up_scale, down_scale):
    stream = stream_in.astype(jnp.float32)
    msq = lax.optimization_barrier(jnp.mean(stream * stream, axis=1))
    shaped = (stream * gain[None, :]).astype(jnp.bfloat16)
    inverse = lax.rsqrt(msq + 1e-06)[:, None]
    gate_full = inverse * gate_scale[None, :] * jnp.dot(shaped, w_gate.astype(jnp.bfloat16), preferred_element_type=jnp.float32)
    up_full = inverse * up_scale[None, :] * jnp.dot(shaped, w_up.astype(jnp.bfloat16), preferred_element_type=jnp.float32)
    hidden = (jax.nn.silu(gate_full) * up_full).astype(jnp.bfloat16)
    down_full = down_scale[None, :] * jnp.dot(hidden, w_down.astype(jnp.bfloat16), preferred_element_type=jnp.float32)
    return (stream + 0.5 * down_full).astype(jnp.bfloat16)

def reference(tokens, first_gain, first_gate, first_up, first_down, first_gate_scale, first_up_scale, first_down_scale, second_gain, second_gate, second_up, second_down, second_gate_scale, second_up_scale, second_down_scale):
    middle = half_step(tokens, first_gain, first_gate, first_up, first_down, first_gate_scale, first_up_scale, first_down_scale)
    return half_step(middle, second_gain, second_gate, second_up, second_down, second_gate_scale, second_up_scale, second_down_scale)
```

```python
import functools
import jax
import jax.numpy as jnp
from jax import lax
from jax.experimental import pallas as pl
from jax.experimental.pallas import tpu as pltpu
from jax.sharding import PartitionSpec as P

MESH = pl.DeviceIdType.MESH
LANES = 128
CHUNK = 32
LAGS = (0, 1, 2, 3, 4, 5, 6, 7, 8)


def bits_of(n):
    return n.bit_length() - 1


def kernel(cfg, *refs):
    ra, cb, chunk, chunks, width, hid, model, lags = cfg
    (tok, gain1, gain2, gsc1, usc1, dsc1, gsc2, usc2, dsc2, g1, u1, d1, g2, u2, d2, out) = refs[:16]
    refs = refs[16:]
    nra, ncb = bits_of(ra), bits_of(cb)
    (fg, fu, fd, wgu, wd, stream, gains, gsc, usc, dsc, sqa, hb, load_sem) = refs[:13]
    refs = refs[13:]
    snd, rcv, own = refs[:nra], refs[nra : 2 * nra], refs[2 * nra : 3 * nra]
    refs = refs[3 * nra :]
    csnd, crcv = refs[0], refs[1]
    rs_s, rs_r, ag_s, ag_r, cb_s, cb_r = refs[2:]
    hl = hid // ra // LANES
    nl = 2 * hl

    me_r = lax.axis_index("ra")
    me_c = lax.axis_index("cb")
    rbit = [(me_r // (1 << k)) % 2 for k in range(nra)]
    cbit = [(me_c // (1 << k)) % 2 for k in range(ncb)]
    ra_peer = [me_r + (1 - 2 * rbit[k]) * (1 << k) for k in range(nra)]
    cb_peer = [me_c + (1 - 2 * cbit[k]) * (1 << k) for k in range(ncb)]
    pos = 0
    for k in range(nra):
        pos = pos + rbit[k] * (1 << (nra - 1 - k))

    loads = []
    for layer, (g, u, d) in enumerate(((g1, u1, d1), (g2, u2, d2))):
        for q, (src, dst) in enumerate(((g, fg), (u, fu), (d, fd))):
            copy = pltpu.make_async_copy(src, dst.at[layer], load_sem.at[layer * 3 + q])
            copy.start()
            loads.append(copy)

    barrier = pltpu.get_barrier_semaphore()
    for k in range(nra):
        pl.semaphore_signal(barrier, inc=1, device_id=(ra_peer[k], me_c), device_id_type=MESH)
    for k in range(ncb):
        pl.semaphore_signal(barrier, inc=1, device_id=(me_r, cb_peer[k]), device_id_type=MESH)

    stream[0] = tok[...]
    gains[0] = gain1[...]
    gains[1] = gain2[...]
    dsc[0] = dsc1[...] * 0.5
    dsc[1] = dsc2[...] * 0.5
    for src, dst, layer in ((gsc1, gsc, 0), (gsc2, gsc, 1), (usc1, usc, 0), (usc2, usc, 1)):
        for i in range(hid // LANES):
            dst[layer, i] = src[i : i + 1, :]

    def rev(j):
        r = 0
        for k in range(nra):
            r |= ((j >> k) & 1) << (nra - 1 - k)
        return r

    hw = hl * LANES

    def convert_cols(layer, src, half):
        for j in range(ra):
            r = rev(j)
            wgu[layer, j, :, half * hw : (half + 1) * hw] = src[layer, :, r * hw : (r + 1) * hw].astype(jnp.bfloat16)

    def convert_down(layer):
        for j in range(ra):
            r = rev(j)
            wd[layer, j * hw : (j + 1) * hw, :] = fd[layer, r * hw : (r + 1) * hw, :].astype(jnp.bfloat16)

    loads[0].wait()
    convert_cols(0, fg, 0)
    loads[1].wait()
    convert_cols(0, fu, 1)
    pl.semaphore_wait(barrier, nra + ncb)

    def rs_copy(k, c):
        return pltpu.make_async_remote_copy(
            src_ref=snd[k].at[c], dst_ref=rcv[k].at[c], send_sem=rs_s.at[k, c], recv_sem=rs_r.at[k, c],
            device_id=(ra_peer[k], me_c), device_id_type=MESH)

    def ag_copy(a, c):
        span = 1 << a
        part = hb.at[c, pl.ds((pos // span) * (span * hl), span * hl)]
        return pltpu.make_async_remote_copy(
            src_ref=part, dst_ref=part, send_sem=ag_s.at[a, c], recv_sem=ag_r.at[a, c],
            device_id=(ra_peer[nra - 1 - a], me_c), device_id_type=MESH)

    def cb_copy(b, i):
        return pltpu.make_async_remote_copy(
            src_ref=csnd.at[b, i], dst_ref=crcv.at[b, i], send_sem=cb_s.at[b, i], recv_sem=cb_r.at[b, i],
            device_id=(me_r, cb_peer[b]), device_id_type=MESH)

    def put_squares(k, c, sq):
        hi = sq.astype(jnp.bfloat16)
        lo = (sq - hi.astype(jnp.float32)).astype(jnp.bfloat16)
        lane = lax.broadcasted_iota(jnp.int32, sq.shape, 1)
        mixed = jnp.where(lane < LANES // 2, hi.astype(jnp.float32), lo.astype(jnp.float32))
        snd[k][c, (ra >> (k + 1)) * nl] = mixed.astype(jnp.bfloat16)

    def get_squares(k, c):
        v = rcv[k][c, (ra >> (k + 1)) * nl].astype(jnp.float32)
        return sqa[c] + (v + pltpu.roll(v, LANES // 2, 1))

    def first(layer, c):
        s = stream[layer, c].astype(jnp.float32)
        sq = jnp.broadcast_to(jnp.sum(s * s, axis=1, keepdims=True), (chunk, LANES))
        sqa[c] = sq
        put_squares(0, c, sq)
        shaped = (s * gains[layer]).astype(jnp.bfloat16)
        half = ra // 2
        for jj in range(half):
            r = jnp.dot(shaped, wgu[layer, (1 - rbit[0]) * half + jj], preferred_element_type=jnp.float32)
            for q in range(nl):
                snd[0][c, jj * nl + q] = r[:, q * LANES : (q + 1) * LANES].astype(jnp.bfloat16)
        rs_copy(0, c).start()
        for jj in range(half):
            r = jnp.dot(shaped, wgu[layer, rbit[0] * half + jj], preferred_element_type=jnp.float32)
            for q in range(nl):
                own[0][c, jj * nl + q] = r[:, q * LANES : (q + 1) * LANES]

    def reduce(k, layer, c):
        rs_copy(k - 1, c).wait()
        n = (ra >> (k + 1)) * nl
        sq = get_squares(k - 1, c)
        sqa[c] = sq
        put_squares(k, c, sq)
        away = pl.ds((1 - rbit[k]) * n, n)
        snd[k][c, 0:n] = (own[k - 1][c, away] + rcv[k - 1][c, away].astype(jnp.float32)).astype(jnp.bfloat16)
        rs_copy(k, c).start()
        keep = pl.ds(rbit[k] * n, n)
        own[k][c] = own[k - 1][c, keep] + rcv[k - 1][c, keep].astype(jnp.float32)

    def gate(layer, c):
        k = nra - 1
        rs_copy(k, c).wait()
        total = own[k][c] + rcv[k][c, 0:nl].astype(jnp.float32)
        inverse = lax.rsqrt(get_squares(k, c) / model + 1e-06)[None]
        mine = pl.ds(me_r * hl, hl)
        g = inverse * gsc[layer, mine] * total[:hl]
        u = inverse * usc[layer, mine] * total[hl:]
        hidden = (g / (1.0 + jnp.exp(-g))) * u
        hb[c, pl.ds(pos * hl, hl)] = hidden.astype(jnp.bfloat16)
        ag_copy(0, c).start()

    def gather(a, layer, c):
        ag_copy(a - 1, c).wait()
        ag_copy(a, c).start()

    def down(layer, c):
        ag_copy(nra - 1, c).wait()
        h = jnp.concatenate([hb[c, i] for i in range(hid // LANES)], axis=1)
        i = layer * chunks + c
        csnd[0, i] = jnp.dot(h, wd[layer], preferred_element_type=jnp.float32).astype(jnp.bfloat16)
        cb_copy(0, i).start()

    def csum(b, i):
        cb_copy(b, i).wait()
        return csnd[b, i].astype(jnp.float32) + crcv[b, i].astype(jnp.float32)

    def across(b, layer, c):
        i = layer * chunks + c
        csnd[b, i] = csum(b - 1, i).astype(jnp.bfloat16)
        cb_copy(b, i).start()

    def last(layer, c):
        i = layer * chunks + c
        total = csum(ncb - 1, i)
        s = stream[layer, c].astype(jnp.float32)
        stream[layer + 1, c] = (s + dsc[layer] * total).astype(jnp.bfloat16)

    stages = [first]
    stages += [functools.partial(reduce, k) for k in range(1, nra)]
    stages += [gate]
    stages += [functools.partial(gather, a) for a in range(1, nra)]
    stages += [down]
    stages += [functools.partial(across, b) for b in range(1, ncb)]
    stages += [last]
    shift = max(chunks, lags[-1] + 1)

    later = {
        0: lambda: (loads[2].wait(), convert_down(0)),
        1: lambda: (loads[3].wait(), convert_cols(1, fg, 0)),
        2: lambda: (loads[4].wait(), convert_cols(1, fu, 1)),
        3: lambda: (loads[5].wait(), convert_down(1)),
    }

    def tick(t, carry):
        order = [0] + list(range(len(stages) - 1, 0, -1))
        for s in order:
            rel = t - lags[s]
            layer = jnp.where(rel >= shift, 1, 0)
            c = rel - layer * shift

            @pl.when((rel >= 0) & (c < chunks))
            def _(s=s, layer=layer, c=c):
                stages[s](layer, c)

        for at, act in later.items():
            @pl.when(t == at)
            def _(act=act):
                act()

        return carry

    lax.fori_loop(0, shift + chunks + lags[-1], tick, 0)
    out[...] = stream[2]


def fused(cfg, *args):
    ra, cb, chunk, chunks, width, hid, model, lags = cfg
    nra, ncb = bits_of(ra), bits_of(cb)
    (tok, gain1, g1, u1, d1, gs1, us1, ds1, gain2, g2, u2, d2, gs2, us2, ds2) = args
    rows = hid // LANES
    nl = 2 * (hid // ra // LANES)
    bf, f32 = jnp.bfloat16, jnp.float32
    V = pltpu.VMEM
    D = pltpu.SemaphoreType.DMA
    scratch = [
        V((2, width, hid), f32),
        V((2, width, hid), f32),
        V((2, hid, width), f32),
        V((2, ra, width, nl * LANES), bf),
        V((2, hid, width), bf),
        V((3, chunks, chunk, width), bf),
        V((2, 1, width), f32),
        V((2, rows, 1, LANES), f32),
        V((2, rows, 1, LANES), f32),
        V((2, 1, width), f32),
        V((chunks, chunk, LANES), f32),
        V((chunks, rows, chunk, LANES), bf),
        D((6,)),
    ]
    scratch += [V((chunks, (ra >> (k + 1)) * nl + 1, chunk, LANES), bf) for k in range(nra)]
    scratch += [V((chunks, (ra >> (k + 1)) * nl + 1, chunk, LANES), bf) for k in range(nra)]
    scratch += [V((chunks, (ra >> (k + 1)) * nl, chunk, LANES), f32) for k in range(nra)]
    scratch += [V((ncb, 2 * chunks, chunk, width), bf), V((ncb, 2 * chunks, chunk, width), bf)]
    scratch += [D((nra, chunks)), D((nra, chunks)), D((nra, chunks)), D((nra, chunks))]
    scratch += [D((ncb, 2 * chunks)), D((ncb, 2 * chunks))]
    vm = pl.BlockSpec(memory_space=pltpu.VMEM)
    hbm = pl.BlockSpec(memory_space=pl.ANY)
    result = pl.pallas_call(
        functools.partial(kernel, cfg),
        out_shape=jax.ShapeDtypeStruct((chunks, chunk, width), bf),
        in_specs=[vm] * 9 + [hbm] * 6,
        out_specs=vm,
        scratch_shapes=scratch,
        compiler_params=pltpu.CompilerParams(collective_id=0, has_side_effects=True, vmem_limit_bytes=64 * 1000 * 1000),
    )(
        tok.reshape(chunks, chunk, width),
        gain1.reshape(1, width), gain2.reshape(1, width),
        gs1.reshape(rows, LANES), us1.reshape(rows, LANES), ds1.reshape(1, width),
        gs2.reshape(rows, LANES), us2.reshape(rows, LANES), ds2.reshape(1, width),
        g1, u1, d1, g2, u2, d2,
    )
    return result.reshape(chunks * chunk, width)


def plain_half(model, s_in, gain, w_gate, w_up, w_down, gate_scale, up_scale, down_scale):
    stream = s_in.astype(jnp.float32)
    squares = jnp.sum(stream * stream, axis=1)
    shaped = (stream * gain[None, :]).astype(jnp.bfloat16)
    gate_part = jnp.dot(shaped, w_gate.astype(jnp.bfloat16), preferred_element_type=jnp.float32)
    up_part = jnp.dot(shaped, w_up.astype(jnp.bfloat16), preferred_element_type=jnp.float32)
    squares, gate_sum, up_sum = lax.psum((squares, gate_part, up_part), "ra")
    inverse = lax.rsqrt(squares / model + 1e-06)[:, None]
    gate_full = inverse * gate_scale[None, :] * gate_sum
    up_full = inverse * up_scale[None, :] * up_sum
    hidden = (jax.nn.silu(gate_full) * up_full).astype(jnp.bfloat16)
    down_part = jnp.dot(hidden, w_down.astype(jnp.bfloat16), preferred_element_type=jnp.float32)
    down_sum = lax.psum(down_part, "cb")
    return (stream + 0.5 * down_scale[None, :] * down_sum).astype(jnp.bfloat16)


def solution(mesh):
    ra, cb = mesh.shape["ra"], mesh.shape["cb"]

    def body(*args):
        tokens, width = args[0].shape
        hid = args[2].shape[1]
        power = ra & (ra - 1) == 0 and cb & (cb - 1) == 0 and ra > 1 and cb > 1
        if power and hid % (ra * LANES) == 0 and width % LANES == 0 and tokens % CHUNK == 0:
            stages = 2 * bits_of(ra) + bits_of(cb) + 1
            lags = LAGS if len(LAGS) == stages else tuple(range(stages))
            cfg = (ra, cb, CHUNK, tokens // CHUNK, width, hid, width * ra, lags)
            return fused(cfg, *args)
        middle = plain_half(width * ra, *args[:8])
        return plain_half(width * ra, middle, *args[8:])

    col, grid, turned = P("ra"), P("ra", "cb"), P("cb", "ra")
    sub = (col, grid, grid, turned, P("cb"), P("cb"), col)
    return jax.shard_map(
        body, mesh=mesh, in_specs=(P(None, "ra"),) + sub + sub, out_specs=P(None, "ra"), check_vma=False)
```

```python
import functools
import jax
import jax.numpy as jnp
from jax import lax
from jax.experimental import pallas as pl
from jax.experimental.pallas import tpu as pltpu
from jax.sharding import PartitionSpec as P

MESH = pl.DeviceIdType.MESH
LANES = 128
CHUNK = 32
TIMES = (0.0, 1.5, 3.0, 4.5, 5.7, 6.9)


def kernel(cfg, *refs):
    ra, cb, chunk, chunks, width, hid, model, times = cfg
    (tok, gain1, gain2, gsc1, usc1, dsc1, gsc2, usc2, dsc2, g1, u1, d1, g2, u2, d2, out) = refs[:16]
    refs = refs[16:]
    far = ra // 2
    (fg, fu, fd, wgu, wd, stream, gains, gsc, usc, dsc, sqa, hb, load_sem) = refs[:13]
    refs = refs[13:]
    ysnd, yrcv, yown, zsnd, zrcv, zown, csnd, crcv = refs[:8]
    y_s, y_r, z_s, z_r, h_s, h_r, w_s, w_r, cb_s, cb_r = refs[8:]
    hl = hid // ra // LANES
    nl = 2 * hl

    me_r = lax.axis_index("ra")
    me_c = lax.axis_index("cb")
    bit, z = me_r % 2, me_r // 2
    pair = z * 2 + 1 - bit
    pos = bit * far + z
    z_of = [(z + d) % far for d in range(far)]
    c_of = [(me_c + d) % cb for d in range(cb)]
    loads = []
    for layer, (g, u, d) in enumerate(((g1, u1, d1), (g2, u2, d2))):
        for q, (src, dst) in enumerate(((g, fg), (u, fu), (d, fd))):
            copy = pltpu.make_async_copy(src, dst.at[layer], load_sem.at[layer * 3 + q])
            copy.start()
            loads.append(copy)

    barrier = pltpu.get_barrier_semaphore()
    pl.semaphore_signal(barrier, inc=1, device_id=(pair, me_c), device_id_type=MESH)
    for d in range(1, far):
        pl.semaphore_signal(barrier, inc=1, device_id=(z_of[d] * 2 + bit, me_c), device_id_type=MESH)
    for d in range(1, cb):
        pl.semaphore_signal(barrier, inc=1, device_id=(me_r, c_of[d]), device_id_type=MESH)

    stream[0] = tok[...]
    gains[0] = gain1[...]
    gains[1] = gain2[...]
    dsc[0] = dsc1[...] * 0.5
    dsc[1] = dsc2[...] * 0.5
    for src, dst, layer in ((gsc1, gsc, 0), (gsc2, gsc, 1), (usc1, usc, 0), (usc2, usc, 1)):
        for i in range(hid // LANES):
            dst[layer, i] = src[i : i + 1, :]

    def rev(j):
        return (j % far) * 2 + j // far

    hw = hl * LANES

    def convert_cols(layer, src, half):
        for j in range(ra):
            r = rev(j)
            wgu[layer, j, :, half * hw : (half + 1) * hw] = src[layer, :, r * hw : (r + 1) * hw].astype(jnp.bfloat16)

    def convert_down(layer):
        for j in range(ra):
            r = rev(j)
            wd[layer, j * hw : (j + 1) * hw, :] = fd[layer, r * hw : (r + 1) * hw, :].astype(jnp.bfloat16)

    loads[0].wait()
    convert_cols(0, fg, 0)
    loads[1].wait()
    convert_cols(0, fu, 1)
    pl.semaphore_wait(barrier, 1 + (far - 1) + (cb - 1))

    def remote(src, dst, send, recv, r, col):
        return pltpu.make_async_remote_copy(
            src_ref=src, dst_ref=dst, send_sem=send, recv_sem=recv, device_id=(r, col), device_id_type=MESH)

    def y_copy(c):
        return remote(ysnd.at[c], yrcv.at[c], y_s.at[c], y_r.at[c], pair, me_c)

    def z_copy(d, c):
        return remote(zsnd.at[d - 1, c], zrcv.at[d - 1, c], z_s.at[d - 1, c], z_r.at[d - 1, c], z_of[d] * 2 + bit, me_c)

    def h_copy(d, c):
        part = hb.at[c, pl.ds(pos * hl, hl)]
        return remote(part, part, h_s.at[d - 1, c], h_r.at[d - 1, c], z_of[d] * 2 + bit, me_c)

    def w_copy(c):
        part = hb.at[c, pl.ds(bit * (far * hl), far * hl)]
        return remote(part, part, w_s.at[c], w_r.at[c], pair, me_c)

    def cb_copy(d, i):
        return remote(csnd.at[i], crcv.at[i, me_c], cb_s.at[d - 1, i], cb_r.at[d - 1, i], me_r, c_of[d])

    def packed(sq):
        hi = sq.astype(jnp.bfloat16).astype(jnp.float32)
        lane = lax.broadcasted_iota(jnp.int32, sq.shape, 1)
        return jnp.where(lane < LANES // 2, hi, sq - hi).astype(jnp.bfloat16)

    def unpacked(v):
        v = v.astype(jnp.float32)
        return v + pltpu.roll(v, LANES // 2, 1)

    def first(layer, c):
        s = stream[layer, c].astype(jnp.float32)
        sq = jnp.broadcast_to(jnp.sum(s * s, axis=1, keepdims=True), (chunk, LANES))
        sqa[c] = sq
        ysnd[c, far * nl] = packed(sq)
        shaped = (s * gains[layer]).astype(jnp.bfloat16)
        half = ra // 2
        for jj in range(half):
            r = jnp.dot(shaped, wgu[layer, (1 - bit) * half + jj], preferred_element_type=jnp.float32)
            for q in range(nl):
                ysnd[c, jj * nl + q] = r[:, q * LANES : (q + 1) * LANES].astype(jnp.bfloat16)
        y_copy(c).start()
        for jj in range(half):
            r = jnp.dot(shaped, wgu[layer, bit * half + jj], preferred_element_type=jnp.float32)
            for q in range(nl):
                yown[c, jj * nl + q] = r[:, q * LANES : (q + 1) * LANES]

    def reduce(layer, c):
        y_copy(c).wait()
        sq = sqa[c] + unpacked(yrcv[c, far * nl])
        sqa[c] = sq
        square = packed(sq)
        for d in range(1, far):
            part = pl.ds(z_of[d] * nl, nl)
            zsnd[d - 1, c, 0:nl] = (yown[c, part] + yrcv[c, part].astype(jnp.float32)).astype(jnp.bfloat16)
            zsnd[d - 1, c, nl] = square
            z_copy(d, c).start()
        part = pl.ds(z * nl, nl)
        zown[c] = yown[c, part] + yrcv[c, part].astype(jnp.float32)

    def gate(layer, c):
        total = zown[c]
        sq = sqa[c]
        for d in range(1, far):
            z_copy(d, c).wait()
            total = total + zrcv[d - 1, c, 0:nl].astype(jnp.float32)
            sq = sq + unpacked(zrcv[d - 1, c, nl])
        inverse = lax.rsqrt(sq / model + 1e-06)[None]
        mine = pl.ds(me_r * hl, hl)
        g = inverse * gsc[layer, mine] * total[:hl]
        u = inverse * usc[layer, mine] * total[hl:]
        hidden = (g / (1.0 + jnp.exp(-g))) * u
        hb[c, pl.ds(pos * hl, hl)] = hidden.astype(jnp.bfloat16)
        for d in range(1, far):
            h_copy(d, c).start()

    def gather(layer, c):
        for d in range(1, far):
            h_copy(d, c).wait()
        w_copy(c).start()

    def down(layer, c):
        w_copy(c).wait()
        h = jnp.concatenate([hb[c, i] for i in range(hid // LANES)], axis=1)
        i = layer * chunks + c
        part = jnp.dot(h, wd[layer], preferred_element_type=jnp.float32).astype(jnp.bfloat16)
        csnd[i] = part
        crcv[i, me_c] = part
        for d in range(1, cb):
            cb_copy(d, i).start()

    def last(layer, c):
        i = layer * chunks + c
        for d in range(1, cb):
            cb_copy(d, i).wait()
        total = crcv[i, 0].astype(jnp.float32)
        for q in range(1, cb):
            total = total + crcv[i, q].astype(jnp.float32)
        s = stream[layer, c].astype(jnp.float32)
        stream[layer + 1, c] = (s + dsc[layer] * total).astype(jnp.bfloat16)

    stages = [first, reduce, gate, gather, down, last]
    lags = [int(x) for x in times]
    order = sorted(range(len(stages)), key=lambda s: times[s] - lags[s])
    shift = max(chunks, lags[-1] + 1)

    later = {
        0: lambda: (loads[2].wait(), convert_down(0)),
        1: lambda: (loads[3].wait(), convert_cols(1, fg, 0)),
        2: lambda: (loads[4].wait(), convert_cols(1, fu, 1)),
        3: lambda: (loads[5].wait(), convert_down(1)),
    }

    def tick(t, carry):
        for s in order:
            rel = t - lags[s]
            layer = jnp.where(rel >= shift, 1, 0)
            c = rel - layer * shift

            @pl.when((rel >= 0) & (c < chunks))
            def _(s=s, layer=layer, c=c):
                stages[s](layer, c)

        for at, act in later.items():
            @pl.when(t == at)
            def _(act=act):
                act()

        return carry

    lax.fori_loop(0, shift + chunks + lags[-1], tick, 0)
    out[...] = stream[2]


def fused(cfg, *args):
    ra, cb, chunk, chunks, width, hid, model, times = cfg
    far = ra // 2
    (tok, gain1, g1, u1, d1, gs1, us1, ds1, gain2, g2, u2, d2, gs2, us2, ds2) = args
    rows = hid // LANES
    nl = 2 * (hid // ra // LANES)
    bf, f32 = jnp.bfloat16, jnp.float32
    V = pltpu.VMEM
    D = pltpu.SemaphoreType.DMA
    scratch = [
        V((2, width, hid), f32),
        V((2, width, hid), f32),
        V((2, hid, width), f32),
        V((2, ra, width, nl * LANES), bf),
        V((2, hid, width), bf),
        V((3, chunks, chunk, width), bf),
        V((2, 1, width), f32),
        V((2, rows, 1, LANES), f32),
        V((2, rows, 1, LANES), f32),
        V((2, 1, width), f32),
        V((chunks, chunk, LANES), f32),
        V((chunks, rows, chunk, LANES), bf),
        D((6,)),
    ]
    scratch += [V((chunks, far * nl + 1, chunk, LANES), bf), V((chunks, far * nl + 1, chunk, LANES), bf)]
    scratch += [V((chunks, far * nl, chunk, LANES), f32)]
    scratch += [V((far - 1, chunks, nl + 1, chunk, LANES), bf), V((far - 1, chunks, nl + 1, chunk, LANES), bf)]
    scratch += [V((chunks, nl, chunk, LANES), f32)]
    scratch += [V((2 * chunks, chunk, width), bf), V((2 * chunks, cb, chunk, width), bf)]
    scratch += [D((chunks,))] * 2 + [D((far - 1, chunks))] * 4 + [D((chunks,))] * 2 + [D((cb - 1, 2 * chunks))] * 2
    vm = pl.BlockSpec(memory_space=pltpu.VMEM)
    hbm = pl.BlockSpec(memory_space=pl.ANY)
    result = pl.pallas_call(
        functools.partial(kernel, cfg),
        out_shape=jax.ShapeDtypeStruct((chunks, chunk, width), bf),
        in_specs=[vm] * 9 + [hbm] * 6,
        out_specs=vm,
        scratch_shapes=scratch,
        compiler_params=pltpu.CompilerParams(collective_id=0, has_side_effects=True, vmem_limit_bytes=64 * 1000 * 1000),
    )(
        tok.reshape(chunks, chunk, width),
        gain1.reshape(1, width), gain2.reshape(1, width),
        gs1.reshape(rows, LANES), us1.reshape(rows, LANES), ds1.reshape(1, width),
        gs2.reshape(rows, LANES), us2.reshape(rows, LANES), ds2.reshape(1, width),
        g1, u1, d1, g2, u2, d2,
    )
    return result.reshape(chunks * chunk, width)


def plain_half(model, s_in, gain, w_gate, w_up, w_down, gate_scale, up_scale, down_scale):
    stream = s_in.astype(jnp.float32)
    squares = jnp.sum(stream * stream, axis=1)
    shaped = (stream * gain[None, :]).astype(jnp.bfloat16)
    gate_part = jnp.dot(shaped, w_gate.astype(jnp.bfloat16), preferred_element_type=jnp.float32)
    up_part = jnp.dot(shaped, w_up.astype(jnp.bfloat16), preferred_element_type=jnp.float32)
    squares, gate_sum, up_sum = lax.psum((squares, gate_part, up_part), "ra")
    inverse = lax.rsqrt(squares / model + 1e-06)[:, None]
    gate_full = inverse * gate_scale[None, :] * gate_sum
    up_full = inverse * up_scale[None, :] * up_sum
    hidden = (jax.nn.silu(gate_full) * up_full).astype(jnp.bfloat16)
    down_part = jnp.dot(hidden, w_down.astype(jnp.bfloat16), preferred_element_type=jnp.float32)
    down_sum = lax.psum(down_part, "cb")
    return (stream + 0.5 * down_scale[None, :] * down_sum).astype(jnp.bfloat16)


def solution(mesh):
    ra, cb = mesh.shape["ra"], mesh.shape["cb"]

    def body(*args):
        tokens, width = args[0].shape
        hid = args[2].shape[1]
        even = ra % 2 == 0 and ra > 2 and cb > 1
        if even and hid % (ra * LANES) == 0 and width % LANES == 0 and tokens % CHUNK == 0:
            cfg = (ra, cb, CHUNK, tokens // CHUNK, width, hid, width * ra, TIMES)
            return fused(cfg, *args)
        middle = plain_half(width * ra, *args[:8])
        return plain_half(width * ra, middle, *args[8:])

    col, grid, turned = P("ra"), P("ra", "cb"), P("cb", "ra")
    sub = (col, grid, grid, turned, P("cb"), P("cb"), col)
    return jax.shard_map(
        body, mesh=mesh, in_specs=(P(None, "ra"),) + sub + sub, out_specs=P(None, "ra"), check_vma=False)
```
